32 devices in a mesh: ep: 8 (over z, x), tp: 4 (over y, core).
Axes of the slice: x: 2, y: 2, z: 4, core: 2. Of those that a mesh axis runs over, the one named last changes fastest.
Arguments:
- queries: bfloat16 [2048, 1536], P('ep', 'tp'), may hold values from -600 to 600
- compressed_key_value: bfloat16 [2048, 512], P('ep'), may hold values from -6 to 6
- rope_key: bfloat16 [2048, 32], P('ep'), may hold values from -6 to 6
- latent_norm_gain: float32 [512], replicated, may hold values from 0.1 to 1.9
- latent_to_key_value: bfloat16 [512, 2048], P(None, 'tp'), may hold values from -0.25 to 0.25
- out_proj: bfloat16 [1024, 2048], P(None, 'tp'), may hold values from -1.5 to 1.5
- moe_input: bfloat16 [2048, 2048], P('ep'), may hold values from -6 to 6
- moe_gain: float32 [2048], replicated, may hold values from 0.1 to 1.9
- routes: int32 [2048, 2], P('ep'), may hold values from 0 to 7, all different within a row; in each aligned block of 256 rows (0 to 255, 256 to 511, ...) at most 96 rows name the same one
- route_weight: float32 [2048, 2], P('ep'), may hold values from 0.2 to 1
- gate_weight: bfloat16 [8, 2048, 4096], P('ep', None, 'tp'), may hold values from -0.125 to 0.125
- up_weight: bfloat16 [8, 2048, 4096], P('ep', None, 'tp'), may hold values from -0.125 to 0.125
- down_weight: bfloat16 [8, 4096, 2048], P('ep', 'tp'), may hold values from -0.09375 to 0.09375
Outputs:
- attention_out: bfloat16 [2048, 2048], P('ep', 'tp')
- expert_out: bfloat16 [2048, 2048], P('ep', 'tp')
The draws below stay inside these ranges and needn't reach their ends.
Inputs may be any that keep to these rules, and one draw needn't show every extreme that they name: `routes`: each row names 2 different experts. In the rows of one device (aligned blocks of 256 rows) no expert is named by more than 96 rows, and in some blocks one expert is named by exactly 96 rows.
All inputs are finite; a program needn't handle non-finite values.
Results may differ from the reference program's by a relative error of at most 0.019.
The reference program's roundings to bfloat16 on the way count: a program that leaves them out, or rounds other values in their place, can miss the bound.
Values may be sent and summed in bfloat16 or wider, within the bound.
A program may use at most 128 MiB of HBM per device.

```python
import math
import jax
import jax.numpy as jnp
import numpy as np
from jax import lax

D = 2048
ATTENTION_HEADS = 16
PLAIN_HEAD_DIM = 64
ROPE = 32
VALUE_HEAD_DIM = 64
LATENT_WIDTH = 512
EXPERT_FF = 4096
TOP = 2
TOK_DEV = 256
MLA_W = 1024
MICRO_TOKENS = 2048
EXPERTS = 8
CAP = 96
N_EP = 8
N_TP = 4


def draw_queries(key, part):
    base_values = jax.random.normal(key, (MICRO_TOKENS, ATTENTION_HEADS * (PLAIN_HEAD_DIM + ROPE)), jnp.float32) * 2.0
    return jnp.clip(base_values, -600.0, 600.0).astype(jnp.bfloat16)


def block_scale(rng, shape, split, low, largest):
    factor_of, own = 1.0, jax.random.fold_in(rng, 6)
    for dim, shards_of in split:
        heights = jnp.exp(jax.random.uniform(jax.random.fold_in(own, dim), (shards_of,), jnp.float32, low / len(split), largest / len(split)))
        factor_of = factor_of * jnp.repeat(heights, shape[dim] // shards_of).reshape([-1 if axis == dim else 1 for axis in range(len(shape))])
    return factor_of


def assign_block(rng, own, number, rows, number_of, top, limit, skew):
    sequence = jax.random.permutation(rng, number_of)
    crowded, usual = shares(number_of, rows * top, limit, skew, True), shares(number_of, rows * top, limit, skew, False)
    places = jnp.arange(number_of)

    def named(sizes, offset_by):
        used = int((sizes > 0).sum())
        fixed = max(1, used // 4)
        shifted = fixed + (places - fixed + offset_by * (used - fixed)) % max(1, number_of - fixed)
        return jnp.zeros((number_of,), jnp.int32).at[sequence[jnp.where(places < fixed, places, shifted)]].set(jnp.asarray(sizes, jnp.int32))

    sizes = jnp.where(number % 4 == 0, named(crowded, number // 4), named(usual, number - number // 4 - 1))
    mixed = jax.random.permutation(jax.random.fold_in(own, 3), number_of)
    source_of, receiver = mixed[0:number_of // 2 * 2:2], mixed[1:number_of // 2 * 2:2]
    room = jnp.minimum(sizes[source_of] - 1, limit - sizes[receiver]) // 2
    room = jnp.where((source_of == sequence[0]) | (receiver == sequence[0]) | (sizes[receiver] == 0), 0, jnp.maximum(room, 0))
    shifted = jax.random.randint(jax.random.fold_in(own, 4), (number_of // 2,), 0, 1 << 20) % (room + 1)
    sizes = sizes.at[source_of].add(-shifted).at[receiver].add(shifted)
    members = jnp.searchsorted(jnp.cumsum(sizes), jnp.arange(rows * top), side="right").astype(jnp.int32)
    table = members.reshape(top, rows).T
    table = table[jax.random.permutation(jax.random.fold_in(own, 1), rows)]
    offset_by = jax.random.randint(jax.random.fold_in(own, 2), (rows, 1), 0, top)
    return jnp.take_along_axis(table, (jnp.arange(top)[None, :] + offset_by) % top, axis=1)


def shares(number_of, total, bound, skew, full):
    portions = [(1 << 20) // math.isqrt(standing ** skew) + 1 for standing in range(1, number_of + 1)]
    largest = bound if full else min(bound, max(-(-total // number_of), total * portions[0] // sum(portions)))
    least = 1 if total - largest >= number_of - 1 else 0
    given, spare = [largest] + [least] * (number_of - 1), total - largest - least * (number_of - 1)
    while spare > 0:
        free = [i for i in range(1, number_of) if given[i] < largest] or [i for i in range(1, number_of) if given[i] < bound]
        mass, remaining = sum([portions[i] for i in free]), spare
        for i in free:
            extra = min(bound - given[i], max(1, remaining * portions[i] // mass), spare)
            given[i] = given[i] + extra
            spare = spare - extra
    return np.array(given)


def bell_draw(stream_key, extent, deviation, limit, pieces=(), held_as=jnp.bfloat16):
    drawn = jax.random.normal(stream_key, extent, jnp.float32) * deviation
    if len(pieces) > 0:
        drawn = block_scale(stream_key, extent, pieces, -0.22, 0.18) * drawn
    return jnp.clip(drawn, min=-limit, max=limit).astype(held_as)


def setup_inputs(seed: int = 0) -> dict:
    key_list = jax.random.split(jax.random.key(seed), 14)
    queries = draw_queries(jax.random.fold_in(key_list[13], 71), 0)
    compressed_key_value = bell_draw(key_list[1], (MICRO_TOKENS, LATENT_WIDTH), 1.0, 6.0, ((0, 8),))
    rope_key = bell_draw(key_list[2], (MICRO_TOKENS, ROPE), 1.0, 6.0, ((0, 8),))
    latent_norm_gain = jnp.clip(1.0 + 0.18 * jax.random.normal(key_list[3], (LATENT_WIDTH,), jnp.float32), 0.1, 1.9)
    latent_to_key_value = bell_draw(key_list[4], (LATENT_WIDTH, ATTENTION_HEADS * (PLAIN_HEAD_DIM + VALUE_HEAD_DIM)), LATENT_WIDTH ** -0.5, 0.25, ((1, 4),))
    out_proj = bell_draw(key_list[5], (MLA_W, D), ATTENTION_HEADS ** -0.5, 1.5, ((1, 4),))
    moe_input = bell_draw(key_list[6], (MICRO_TOKENS, D), 1.0, 6.0, ((0, 8),))
    moe_gain = jnp.clip(1.0 + 0.18 * jax.random.normal(key_list[7], (D,), jnp.float32), 0.1, 1.9)
    routes_keys = jax.random.split(jax.random.fold_in(key_list[8], 1), MICRO_TOKENS // TOK_DEV)
    routes_turns = jax.random.permutation(jax.random.fold_in(key_list[8], 3), MICRO_TOKENS // TOK_DEV)
    routes = jax.vmap(lambda own, number: assign_block(jax.random.fold_in(key_list[8], 2), own, number, TOK_DEV, EXPERTS, TOP, CAP, 2))(routes_keys, routes_turns).reshape((MICRO_TOKENS, TOP))
    route_weight = jnp.clip(0.2 + 0.8 * jax.random.uniform(key_list[9], (MICRO_TOKENS, TOP), jnp.float32) ** block_scale(key_list[9], (MICRO_TOKENS, TOP), ((0, 8),), -0.2, 0.2), 0.2, 1.0)
    gate_weight = bell_draw(key_list[10], (EXPERTS, D, EXPERT_FF), D ** -0.5, 0.125, ((0, 8), (2, 4)))
    up_weight = bell_draw(key_list[11], (EXPERTS, D, EXPERT_FF), D ** -0.5, 0.125, ((0, 8), (2, 4)))
    down_weight = bell_draw(key_list[12], (EXPERTS, EXPERT_FF, D), EXPERT_FF ** -0.5, 0.09375, ((0, 8), (1, 4)))
    return {"queries": queries, "compressed_key_value": compressed_key_value, "rope_key": rope_key, "latent_norm_gain": latent_norm_gain, "latent_to_key_value": latent_to_key_value, "out_proj": out_proj, "moe_input": moe_input, "moe_gain": moe_gain, "routes": routes, "route_weight": route_weight, "gate_weight": gate_weight, "up_weight": up_weight, "down_weight": down_weight}


EPSILON = 1e-06
ROPE_BASE_VALUE = 10000.0

def rms_scale(values, gain_vector):
    floats = values.astype(jnp.float32)
    return floats * lax.rsqrt(lax.optimization_barrier(jnp.mean(floats * floats, axis=-1, keepdims=True)) + EPSILON) * gain_vector.astype(jnp.float32)

def rotary(values, positions):
    full_width = values.shape[-1]
    half_dim = full_width // 2
    frequency = ROPE_BASE_VALUE ** (-jnp.arange(half_dim, dtype=jnp.float32) * 2.0 / full_width)
    angles = positions[..., None] * frequency
    cosine = jnp.cos(angles)
    sine_part = jnp.sin(angles)
    first_half = values[..., :half_dim]
    second_half = values[..., half_dim:]
    return jnp.concatenate([first_half * cosine - second_half * sine_part, second_half * cosine + first_half * sine_part], axis=-1)

def slot_table(block_routes, capacity, experts):
    flat_routes = block_routes.reshape(-1).astype(jnp.int32)
    onehot_table = (flat_routes[:, None] == jnp.arange(experts, dtype=jnp.int32)[None, :]).astype(jnp.int32)
    earlier = jnp.cumsum(onehot_table, axis=0) - onehot_table
    slot_index = lax.optimization_barrier(jnp.sum(earlier * onehot_table, axis=1)).astype(jnp.int32)
    destination = (flat_routes * capacity + slot_index).astype(jnp.int32)
    token_count = block_routes.shape[0]
    source_rows = (jnp.arange(flat_routes.shape[0], dtype=jnp.int32) // block_routes.shape[1]).astype(jnp.int32)
    source_table = jnp.full((experts * capacity,), token_count, jnp.int32).at[destination].set(source_rows)
    return (destination, source_table)

def reference(queries, compressed_key_value, rope_key, latent_norm_gain, latent_to_key_value, out_proj, moe_input, moe_gain, routes, route_weight, gate_weight, up_weight, down_weight):
    positions = jnp.arange(MICRO_TOKENS, dtype=jnp.float32)
    query_heads = queries.reshape(MICRO_TOKENS, ATTENTION_HEADS, PLAIN_HEAD_DIM + ROPE)
    query_nope = query_heads[..., :PLAIN_HEAD_DIM]
    query_rope = rotary(query_heads[..., PLAIN_HEAD_DIM:].astype(jnp.float32), positions[:, None]).astype(jnp.bfloat16)
    latent_normed = rms_scale(compressed_key_value, latent_norm_gain).astype(jnp.bfloat16)
    key_value = jnp.dot(latent_normed, latent_to_key_value, preferred_element_type=jnp.float32).astype(jnp.bfloat16)
    key_value = key_value.reshape(MICRO_TOKENS, ATTENTION_HEADS, PLAIN_HEAD_DIM + VALUE_HEAD_DIM)
    key_rope = rotary(rope_key.astype(jnp.float32), positions).astype(jnp.bfloat16)
    score_scale = (PLAIN_HEAD_DIM + ROPE) ** (-0.5)

    def one_head(inputs):
        head_nope, head_rope, head_kv = inputs
        key_nope = head_kv[:, :PLAIN_HEAD_DIM]
        head_values = head_kv[:, PLAIN_HEAD_DIM:]

        def one_block(block_inputs):
            block_nope, block_rope = block_inputs
            scores = (jnp.dot(block_nope, key_nope.T, preferred_element_type=jnp.float32) + jnp.dot(block_rope, key_rope.T, preferred_element_type=jnp.float32)) * score_scale
            row_max = lax.optimization_barrier(jnp.max(scores, axis=-1, keepdims=True))
            weights = jnp.exp(scores - row_max)
            row_total = lax.optimization_barrier(jnp.sum(weights, axis=-1, keepdims=True))
            mixed_rows = jnp.dot(weights.astype(jnp.bfloat16), head_values, preferred_element_type=jnp.float32) / row_total
            return mixed_rows.astype(jnp.bfloat16)
        blocks_out = lax.map(one_block, (head_nope.reshape(N_EP, TOK_DEV, PLAIN_HEAD_DIM), head_rope.reshape(N_EP, TOK_DEV, ROPE)))
        return blocks_out.reshape(MICRO_TOKENS, VALUE_HEAD_DIM)
    per_head = lax.map(one_head, (query_nope.transpose(1, 0, 2), query_rope.transpose(1, 0, 2), key_value.transpose(1, 0, 2)))
    attended = per_head.transpose(1, 0, 2).reshape(MICRO_TOKENS, ATTENTION_HEADS * VALUE_HEAD_DIM)
    attention_out = jnp.dot(attended, out_proj, preferred_element_type=jnp.float32).astype(jnp.bfloat16)
    normed = rms_scale(moe_input, moe_gain).astype(jnp.bfloat16)
    destination, source_table = jax.vmap(lambda block_routes: slot_table(block_routes, CAP, EXPERTS))(routes.reshape(N_EP, TOK_DEV, TOP))
    padded = jnp.concatenate([normed.reshape(N_EP, TOK_DEV, D), jnp.zeros((N_EP, 1, D), jnp.bfloat16)], axis=1)
    outgoing = jax.vmap(lambda table_rows, row_index: table_rows[row_index])(padded, source_table)
    per_expert = outgoing.reshape(N_EP, EXPERTS, CAP, D).transpose(1, 0, 2, 3).reshape(EXPERTS, N_EP * CAP, D)
    width_block = EXPERT_FF // N_TP

    def one_expert(inputs):
        expert_rows, gate_matrix, up_matrix, down_matrix = inputs
        gate_value = jnp.dot(expert_rows, gate_matrix, preferred_element_type=jnp.float32)
        up_value = jnp.dot(expert_rows, up_matrix, preferred_element_type=jnp.float32)
        hidden = (jax.nn.silu(gate_value) * up_value).astype(jnp.bfloat16)
        partial_sums = jnp.einsum('rjf,jfd->jrd', hidden.reshape(-1, N_TP, width_block).astype(jnp.float32), down_matrix.reshape(N_TP, width_block, D).astype(jnp.float32))
        rounded = lax.optimization_barrier(partial_sums.astype(jnp.bfloat16))
        return lax.optimization_barrier(jnp.sum(rounded.astype(jnp.float32), axis=0)).astype(jnp.bfloat16)
    results = lax.map(one_expert, (per_expert, gate_weight, up_weight, down_weight))
    returned = results.reshape(EXPERTS, N_EP, CAP, D).transpose(1, 0, 2, 3).reshape(N_EP, EXPERTS * CAP, D)
    picked = jax.vmap(lambda table_rows, row_index: table_rows[row_index])(returned, destination)
    weighted = picked.astype(jnp.float32).reshape(N_EP, TOK_DEV, TOP, D) * route_weight.reshape(N_EP, TOK_DEV, TOP, 1)
    expert_out = lax.optimization_barrier(jnp.sum(weighted, axis=2)).reshape(MICRO_TOKENS, D).astype(jnp.bfloat16)
    return (attention_out, expert_out)
```

```python
import functools

import jax
import jax.numpy as jnp
from jax import lax
from jax.experimental import pallas as pl
from jax.experimental.pallas import tpu as pltpu
from jax.sharding import PartitionSpec as P

PLAIN_HEAD_DIM = 64
ROPE = 32
VALUE_HEAD_DIM = 64
LANES = 128
CORES = 2
RELAY_GROUPS = 4
CHUNKS = 2


EPSILON = 1e-06
ROPE_BASE_VALUE = 10000.0


def rms_scale(values, gain_vector):
    floats = values.astype(jnp.float32)
    return (
        floats
        * lax.rsqrt(jnp.mean(floats * floats, axis=-1, keepdims=True) + EPSILON)
        * gain_vector
    )


def rotary(values, positions):
    full_width = values.shape[-1]
    half_dim = full_width // 2
    frequency = ROPE_BASE_VALUE ** (-jnp.arange(half_dim, dtype=jnp.float32) * 2.0 / full_width)
    angles = positions[..., None] * frequency
    cosine = jnp.cos(angles)
    sine_part = jnp.sin(angles)
    first_half = values[..., :half_dim]
    second_half = values[..., half_dim:]
    return jnp.concatenate(
        [
            first_half * cosine - second_half * sine_part,
            second_half * cosine + first_half * sine_part,
        ],
        axis=-1,
    )


def merge_rows(block):
    return block.reshape(block.shape[0] * block.shape[1], block.shape[2])


def fused(
    n_ep,
    n_tp,
    heads,
    scale,
    q_ref,
    lat_ref,
    wkv_ref,
    wo_ref,
    moe_ref,
    wg_hbm,
    wu_hbm,
    wd_hbm,
    att_out,
    back,
    wg,
    wu,
    wd,
    g_lat,
    g_moe,
    g_att,
    kv,
    hidden,
    part,
    r1,
    s2,
    r2,
    tot,
    wsem,
    loc_sem,
    lat_a,
    lat_y,
    lat_c,
    moe_a,
    moe_y,
    moe_c,
    att_y,
    att_c,
    red_c,
    red_y,
    ret_a,
):
    me = lax.axis_index("ep")
    tp = lax.axis_index("tp")
    n_y = n_tp // CORES
    my_y = tp // CORES
    my_c = lax.rem(tp, CORES)
    mate = my_y * CORES + (1 - my_c)
    groups = min(RELAY_GROUPS, n_ep)
    per = n_ep // groups
    sends = []

    def to(src, dst, sems, index, ep_id, tp_id):
        copy = pltpu.make_async_remote_copy(
            src_ref=src,
            dst_ref=dst,
            send_sem=sems.at[(0,) + index],
            recv_sem=sems.at[(1,) + index],
            device_id=(ep_id, tp_id),
            device_id_type=pl.DeviceIdType.MESH,
        )
        copy.start()
        sends.append(copy)
        return copy

    barrier = pltpu.get_barrier_semaphore()
    for d in range(1, n_ep):
        pl.semaphore_signal(
            barrier,
            inc=1,
            device_id=(lax.rem(me + d, n_ep), tp),
            device_id_type=pl.DeviceIdType.MESH,
        )
    for d in range(1, n_tp):
        pl.semaphore_signal(
            barrier,
            inc=1,
            device_id=(me, lax.rem(tp + d, n_tp)),
            device_id_type=pl.DeviceIdType.MESH,
        )
    pl.semaphore_wait(barrier, n_ep + n_tp - 2)

    def scatter(kind, buffer, sems, source):
        copies = [pltpu.make_async_copy(source(me), buffer.at[tp, 0], loc_sem.at[kind])]
        copies[0].start()
        for d in range(1, n_ep):
            peer = lax.rem(me + d, n_ep)
            copies.append(to(source(peer), buffer.at[tp, d], sems, (d,), peer, tp))
        return copies

    lat_in = scatter(0, g_lat, lat_a, lambda peer: lat_ref)
    moe_in = scatter(1, g_moe, moe_a, lambda peer: moe_ref.at[peer])
    weights = []
    for i, (source, target) in enumerate(((wg_hbm, wg), (wu_hbm, wu), (wd_hbm, wd))):
        copy = pltpu.make_async_copy(source, target, wsem.at[i])
        copy.start()
        weights.append(copy)

    class Relay:
        def __init__(self, copies, buffer, ysem, csem):
            self.copies, self.buffer, self.ysem, self.csem = copies, buffer, ysem, csem
            self.y, self.c = {}, {}

        def view(self, t, g):
            return self.buffer.at[t, pl.ds(g * per, per)]

        def spread(self, g):
            for d in range(g * per, (g + 1) * per):
                if d == 0:
                    self.copies[0].wait()
                else:
                    self.copies[d].wait_recv()
            self.y[g] = []
            for o in range(1, n_y):
                other = lax.rem(my_y + o, n_y) * CORES + my_c
                self.y[g].append(
                    to(self.view(tp, g), self.view(tp, g), self.ysem, (o, g), me, other)
                )
            self.c[g] = [to(self.view(tp, g), self.view(tp, g), self.csem, (0, g), me, mate)]

        def forward(self, g):
            for o in range(1, n_y):
                self.y[g][o - 1].wait_recv()
                came = lax.rem(my_y + n_y - o, n_y) * CORES + my_c
                self.c[g].append(
                    to(self.view(came, g), self.view(came, g), self.csem, (o, g), me, mate)
                )

        def finish(self, g):
            for copy in self.c[g]:
                copy.wait_recv()

    lat = Relay(lat_in, g_lat, lat_y, lat_c)
    moe = Relay(moe_in, g_moe, moe_y, moe_c)
    for g in range(groups):
        lat.spread(g)
        if g > 0:
            lat.forward(g - 1)
    lat.forward(groups - 1)
    for g in range(groups):
        lat.finish(g)
    moe.spread(0)

    block = n_ep * lat_ref.shape[0]
    latent = wkv_ref.shape[0]

    def expand(t, carry):
        rows = merge_rows(g_lat[t])
        kv[pl.ds(pl.multiple_of(t * block, block), block), :] = jnp.dot(
            rows[:, :latent], wkv_ref[...], preferred_element_type=jnp.float32
        ).astype(jnp.bfloat16)
        return carry

    lax.fori_loop(0, n_tp, expand, 0)
    whole_lat = g_lat.reshape(n_tp * block, g_lat.shape[3])
    row_block = q_ref.shape[0]
    step = 0
    pending = [lambda g=g: moe.spread(g) for g in range(1, groups)]
    done_heads = []
    lane = lax.broadcasted_iota(jnp.int32, (1, LANES), 1)
    for h in range(heads):
        head = kv[:, h * LANES : (h + 1) * LANES]
        keys = jnp.where(lane < PLAIN_HEAD_DIM, head, whole_lat[:, latent : latent + LANES])
        scores = (
            lax.dot_general(
                q_ref[:, h * LANES : (h + 1) * LANES],
                keys,
                (((1,), (1,)), ((), ())),
                preferred_element_type=jnp.float32,
            )
            * scale
        )
        top = jnp.max(scores, axis=-1, keepdims=True)
        e = jnp.exp(scores - top)
        total = jnp.sum(e, axis=-1, keepdims=True)
        mixed = (
            jnp.dot(e.astype(jnp.bfloat16), head, preferred_element_type=jnp.float32) / total
        )
        if heads % 2 == 0:
            if h % 2 == 0:
                held = pltpu.roll(mixed, VALUE_HEAD_DIM, 1)
            else:
                g_att[tp, :, (h // 2) * LANES : (h // 2 + 1) * LANES] = jnp.where(
                    lane < VALUE_HEAD_DIM, held, mixed
                ).astype(jnp.bfloat16)
        else:
            g_att[tp, :, h * LANES : (h + 1) * LANES] = jnp.where(
                lane < PLAIN_HEAD_DIM, 0.0, mixed
            ).astype(jnp.bfloat16)
        if pending:
            pending.pop(0)()
            moe.forward(groups - len(pending) - 2)
    while pending:
        pending.pop(0)()
        moe.forward(groups - len(pending) - 2)
    moe.forward(groups - 1)

    own = g_att.at[tp]
    att_in = []
    for o in range(1, n_y):
        att_in.append(
            to(own, own, att_y, (o,), me, lax.rem(my_y + o, n_y) * CORES + my_c)
        )
    att_mate = [to(own, own, att_c, (0,), me, mate)]

    slots = n_ep // CHUNKS
    cap = moe_ref.shape[1]
    rows = slots * cap
    columns = moe_ref.shape[2]
    ff = wg.shape[1]
    tile = min(256, ff)

    def up(c):
        for g in range(groups):
            if (g * per) // slots == c:
                moe.finish(g)

        def one(f, carry):
            span = pl.ds(pl.multiple_of(f * tile, tile), tile)
            gate = jnp.zeros((rows, tile), jnp.float32)
            lift = jnp.zeros((rows, tile), jnp.float32)
            for t in range(n_tp):
                x = merge_rows(g_moe[t, c * slots : (c + 1) * slots])
                gate += jnp.dot(
                    x, wg[t * columns : (t + 1) * columns, span], preferred_element_type=jnp.float32
                )
                lift += jnp.dot(
                    x, wu[t * columns : (t + 1) * columns, span], preferred_element_type=jnp.float32
                )
            hidden[:, span] = (gate / (1.0 + jnp.exp(-gate)) * lift).astype(jnp.bfloat16)
            return carry

        lax.fori_loop(0, ff // tile, one, 0)

    def down(c):
        def one(t, carry):
            span = pl.ds(pl.multiple_of(t * columns, columns), columns)
            part[t, c * slots : (c + 1) * slots] = (
                jnp.dot(hidden[...], wd[:, span], preferred_element_type=jnp.float32)
                .astype(jnp.bfloat16)
                .reshape(slots, cap, columns)
            )
            return carry

        lax.fori_loop(0, n_tp, one, 0)

    reduce_c, reduce_y = {}, {}

    def swap(c):
        span = pl.ds(c * slots, slots)
        for o in list(range(1, n_y)) + [0]:
            y = lax.rem(my_y + o, n_y)
            reduce_c[c, o] = to(
                part.at[y * CORES + (1 - my_c), span], r1.at[o, span], red_c, (o, c), me, mate
            )

    def level_two(c):
        span = pl.ds(c * slots, slots)
        for o in range(1, n_y):
            y = lax.rem(my_y + o, n_y)
            reduce_c[c, o].wait_recv()
            s2[o, span] = (
                part[y * CORES + my_c, span].astype(jnp.float32) + r1[o, span].astype(jnp.float32)
            ).astype(jnp.bfloat16)
            reduce_y[c, o] = to(
                s2.at[o, span], r2.at[o, span], red_y, (o, c), me, y * CORES + my_c
            )

    returns = []

    def give_back(c):
        span = pl.ds(c * slots, slots)
        reduce_c[c, 0].wait_recv()
        total = part[tp, span].astype(jnp.float32) + r1[0, span].astype(jnp.float32)
        for o in range(1, n_y):
            reduce_y[c, o].wait_recv()
            total += r2[o, span].astype(jnp.float32)
        tot[span] = total.astype(jnp.bfloat16)
        for d in range(c * slots, (c + 1) * slots):
            if d == 0:
                back[0] = tot[0]
            else:
                peer = lax.rem(me + n_ep - d, n_ep)
                returns.append(to(tot.at[d], back.at[d], ret_a, (d,), peer, tp))

    def att_forward():
        for o in range(1, n_y):
            att_in[o - 1].wait_recv()
            came = g_att.at[lax.rem(my_y + n_y - o, n_y) * CORES + my_c]
            att_mate.append(to(came, came, att_c, (o,), me, mate))

    def project():
        for copy in att_mate:
            copy.wait_recv()
        width = g_att.shape[2]
        total = jnp.zeros(att_out.shape, jnp.float32)
        for t in range(n_tp):
            total += jnp.dot(
                g_att[t], wo_ref[t * width : (t + 1) * width, :], preferred_element_type=jnp.float32
            )
        att_out[...] = total.astype(jnp.bfloat16)

    for copy in weights:
        copy.wait()
    for c in range(CHUNKS):
        up(c)
        if c == 0:
            att_forward()
        if c > 0:
            level_two(c - 1)
        down(c)
        swap(c)
        if c > 0:
            give_back(c - 1)
    level_two(CHUNKS - 1)
    project()
    give_back(CHUNKS - 1)
    for copy in returns:
        copy.wait_recv()
    for copy in sends:
        copy.wait_send()


def local(
    queries,
    compressed_key_value,
    rope_key,
    latent_norm_gain,
    latent_to_key_value,
    out_proj,
    moe_input,
    moe_gain,
    routes,
    route_weight,
    gate_weight,
    up_weight,
    down_weight,
):
    n_ep = lax.axis_size("ep")
    n_tp = lax.axis_size("tp")
    me = lax.axis_index("ep")
    tp = lax.axis_index("tp")
    n_y = n_tp // CORES
    bf16 = jnp.bfloat16
    row_count = queries.shape[0]
    heads = latent_to_key_value.shape[1] // (PLAIN_HEAD_DIM + VALUE_HEAD_DIM)
    latent = compressed_key_value.shape[1]
    positions = (me * row_count + jnp.arange(row_count, dtype=jnp.int32)).astype(jnp.float32)
    q_heads = queries.reshape(row_count, heads, PLAIN_HEAD_DIM + ROPE)
    q_rope = rotary(q_heads[..., PLAIN_HEAD_DIM:].astype(jnp.float32), positions[:, None])
    pad = LANES - PLAIN_HEAD_DIM - ROPE
    q_all = jnp.concatenate(
        [
            q_heads[..., :PLAIN_HEAD_DIM],
            q_rope.astype(bf16),
            jnp.zeros((row_count, heads, pad), bf16),
        ],
        axis=-1,
    ).reshape(row_count, heads * LANES)
    share = row_count // n_tp
    cut = lambda x: lax.dynamic_slice_in_dim(x, tp * share, share, 0)
    lat = jnp.concatenate(
        [
            rms_scale(cut(compressed_key_value), latent_norm_gain).astype(bf16),
            jnp.zeros((share, PLAIN_HEAD_DIM), bf16),
            rotary(cut(rope_key).astype(jnp.float32), cut(positions)).astype(bf16),
            jnp.zeros((share, pad), bf16),
        ],
        axis=1,
    )
    if heads % 2 == 0:
        wo = out_proj
        att_width = heads * VALUE_HEAD_DIM
    else:
        wo = out_proj.reshape(n_tp * heads, VALUE_HEAD_DIM, out_proj.shape[1])
        wo = jnp.concatenate([jnp.zeros_like(wo), wo], axis=1)
        wo = wo.reshape(n_tp * heads * LANES, out_proj.shape[1])
        att_width = heads * LANES

    moe_rows, model_width = moe_input.shape
    top = routes.shape[1]
    capacity = 3 * moe_rows // n_ep
    places = -(-capacity // 16) * 16
    columns = model_width // n_tp
    flat = routes.reshape(-1)
    hot = (flat[:, None] == jnp.arange(n_ep, dtype=jnp.int32)[None, :]).astype(bf16)
    pairs = flat.shape[0]
    before = jnp.tril(jnp.ones((pairs, pairs), bf16), -1)
    earlier = jnp.dot(before, hot, preferred_element_type=jnp.float32)
    slot = jnp.sum(earlier * hot.astype(jnp.float32), axis=1).astype(jnp.int32)
    destination = (flat * places + slot).reshape(moe_rows, top)
    normed = rms_scale(moe_input, moe_gain).astype(bf16)
    own_normed = lax.dynamic_slice_in_dim(normed, tp * columns, columns, 1)
    place = jnp.arange(n_ep * places, dtype=jnp.int32)
    choose = jnp.zeros((n_ep * places, moe_rows), jnp.bool_)
    for k in range(top):
        choose = choose | (place[:, None] == destination[:, k][None, :])
    outgoing = jnp.dot(
        choose.astype(bf16), own_normed, preferred_element_type=jnp.float32
    ).astype(bf16)
    outgoing = outgoing.reshape(n_ep, places, columns)

    ff = gate_weight.shape[2]
    groups = min(RELAY_GROUPS, n_ep)
    vmem = pl.BlockSpec(memory_space=pltpu.VMEM)
    hbm = pl.BlockSpec(memory_space=pltpu.HBM)
    dma = lambda *shape: pltpu.SemaphoreType.DMA((2,) + shape)
    attention_out, back = pl.pallas_call(
        functools.partial(fused, n_ep, n_tp, heads, (PLAIN_HEAD_DIM + ROPE) ** (-0.5)),
        out_shape=(
            jax.ShapeDtypeStruct((row_count, out_proj.shape[1]), bf16),
            jax.ShapeDtypeStruct((n_ep, places, columns), bf16),
        ),
        in_specs=[vmem] * 5 + [hbm] * 3,
        out_specs=(vmem, vmem),
        scratch_shapes=[
            pltpu.VMEM((model_width, ff), bf16),
            pltpu.VMEM((model_width, ff), bf16),
            pltpu.VMEM((ff, model_width), bf16),
            pltpu.VMEM((n_tp, n_ep, share, latent + LANES), bf16),
            pltpu.VMEM((n_tp, n_ep, places, columns), bf16),
            pltpu.VMEM((n_tp, row_count, att_width), bf16),
            pltpu.VMEM((n_ep * row_count, heads * LANES), bf16),
            pltpu.VMEM((n_ep // CHUNKS * places, ff), bf16),
            pltpu.VMEM((n_tp, n_ep, places, columns), bf16),
            pltpu.VMEM((n_y, n_ep, places, columns), bf16),
            pltpu.VMEM((n_y, n_ep, places, columns), bf16),
            pltpu.VMEM((n_y, n_ep, places, columns), bf16),
            pltpu.VMEM((n_ep, places, columns), bf16),
            pltpu.SemaphoreType.DMA((3,)),
            pltpu.SemaphoreType.DMA((2,)),
            dma(n_ep),
            dma(n_y, groups),
            dma(n_y, groups),
            dma(n_ep),
            dma(n_y, groups),
            dma(n_y, groups),
            dma(n_y),
            dma(n_y),
            dma(n_y, CHUNKS),
            dma(n_y, CHUNKS),
            dma(n_ep),
        ],
        compiler_params=pltpu.CompilerParams(
            collective_id=0, has_side_effects=True, vmem_limit_bytes=60 * 1024 * 1024
        ),
        name="fused",
    )(
        q_all,
        lat,
        latent_to_key_value,
        wo,
        outgoing,
        gate_weight.reshape(model_width, ff),
        up_weight.reshape(model_width, ff),
        down_weight.reshape(ff, model_width),
    )
    flat_back = back.reshape(n_ep * places, columns)
    near = lax.rem(routes - me + n_ep, n_ep) * places + slot.reshape(moe_rows, top)
    expert_out = jnp.zeros((moe_rows, columns), jnp.float32)
    for k in range(top):
        pick = (near[:, k][:, None] == place[None, :]).astype(bf16)
        picked = jnp.dot(pick, flat_back, preferred_element_type=jnp.float32)
        expert_out = expert_out + picked * route_weight[:, k][:, None]
    return (attention_out, expert_out.astype(bf16))


def solution(mesh):
    return jax.shard_map(
        local,
        mesh=mesh,
        in_specs=(
            P("ep", "tp"),
            P("ep", None),
            P("ep", None),
            P(),
            P(None, "tp"),
            P(None, "tp"),
            P("ep", None),
            P(),
            P("ep", None),
            P("ep", None),
            P("ep", None, "tp"),
            P("ep", None, "tp"),
            P("ep", "tp", None),
        ),
        out_specs=(P("ep", "tp"), P("ep", "tp")),
        check_vma=False,
    )
```

```python
import functools

import jax
import jax.numpy as jnp
from jax import lax
from jax.experimental import pallas as pl
from jax.experimental.pallas import tpu as pltpu
from jax.sharding import PartitionSpec as P

PLAIN_HEAD_DIM = 64
ROPE = 32
VALUE_HEAD_DIM = 64
LANES = 128
CORES = 2
RELAY_GROUPS = 4
CHUNKS = 2


EPSILON = 1e-06
ROPE_BASE_VALUE = 10000.0


def rms_scale(values, gain_vector):
    floats = values.astype(jnp.float32)
    return (
        floats
        * lax.rsqrt(jnp.mean(floats * floats, axis=-1, keepdims=True) + EPSILON)
        * gain_vector
    )


def rotary(values, positions):
    full_width = values.shape[-1]
    half_dim = full_width // 2
    frequency = ROPE_BASE_VALUE ** (-jnp.arange(half_dim, dtype=jnp.float32) * 2.0 / full_width)
    angles = positions[..., None] * frequency
    cosine = jnp.cos(angles)
    sine_part = jnp.sin(angles)
    first_half = values[..., :half_dim]
    second_half = values[..., half_dim:]
    return jnp.concatenate(
        [
            first_half * cosine - second_half * sine_part,
            second_half * cosine + first_half * sine_part,
        ],
        axis=-1,
    )


def ep_shape(n_ep):
    nx = 2 if n_ep % 2 == 0 else 1
    nz = n_ep // nx
    order = [0] if nz == 1 else [0, nz // 2] + [d for d in range(1, nz) if d != nz // 2]
    return nx, nz, order


def merge_rows(block):
    return block.reshape(block.shape[0] * block.shape[1], block.shape[2])


def fused(
    n_ep,
    n_tp,
    heads,
    scale,
    q_ref,
    lat_ref,
    wkv_ref,
    wo_ref,
    moe_ref,
    wg_hbm,
    wu_hbm,
    wd_hbm,
    att_out,
    back,
    wg,
    wu,
    wd,
    g_lat,
    g_moe,
    g_att,
    kv,
    hidden,
    part,
    r1,
    s2,
    r2,
    tot,
    wsem,
    loc_sem,
    lat_a,
    lat_x,
    lat_c,
    moe_a,
    moe_y,
    moe_c,
    att_y,
    att_c,
    red_c,
    red_y,
    ret_a,
):
    me = lax.axis_index("ep")
    tp = lax.axis_index("tp")
    n_y = n_tp // CORES
    my_y = tp // CORES
    my_c = lax.rem(tp, CORES)
    mate = my_y * CORES + (1 - my_c)
    groups = min(RELAY_GROUPS, n_ep)
    per = n_ep // groups
    nx, nz, order = ep_shape(n_ep)
    my_z = me // nx
    my_x = lax.rem(me, nx)
    sends = []

    def ahead(s):
        z = lax.rem(my_z + order[s // nx], nz)
        return z * nx + lax.rem(my_x + s % nx, nx)

    def behind(s):
        z = lax.rem(my_z + nz - order[s // nx], nz)
        return z * nx + lax.rem(my_x + nx - s % nx, nx)

    def to(src, dst, sems, index, ep_id, tp_id):
        copy = pltpu.make_async_remote_copy(
            src_ref=src,
            dst_ref=dst,
            send_sem=sems.at[(0,) + index],
            recv_sem=sems.at[(1,) + index],
            device_id=(ep_id, tp_id),
            device_id_type=pl.DeviceIdType.MESH,
        )
        copy.start()
        sends.append(copy)
        return copy

    barrier = pltpu.get_barrier_semaphore()
    for d in range(1, n_ep):
        pl.semaphore_signal(
            barrier,
            inc=1,
            device_id=(lax.rem(me + d, n_ep), tp),
            device_id_type=pl.DeviceIdType.MESH,
        )
    for d in range(1, n_tp):
        pl.semaphore_signal(
            barrier,
            inc=1,
            device_id=(me, lax.rem(tp + d, n_tp)),
            device_id_type=pl.DeviceIdType.MESH,
        )
    pl.semaphore_wait(barrier, n_ep + n_tp - 2)

    moe_in = [pltpu.make_async_copy(moe_ref.at[me], g_moe.at[tp, 0], loc_sem.at[1])]
    moe_in[0].start()
    for s in range(1, n_ep):
        moe_in.append(to(moe_ref.at[ahead(s)], g_moe.at[tp, s], moe_a, (s,), ahead(s), tp))
    own_lat = my_c * nx
    lat_in = [pltpu.make_async_copy(lat_ref, g_lat.at[own_lat, 0], loc_sem.at[0])]
    lat_in[0].start()
    for i in range(1, nz):
        lat_in.append(
            to(lat_ref, g_lat.at[own_lat, i], lat_a, (i,), ahead(i * nx), tp)
        )
    lat_over = []

    def lat_relay(steps):
        for i in steps:
            if i == 0:
                lat_in[0].wait()
            else:
                lat_in[i].wait_recv()
            mine = g_lat.at[own_lat, i]
            lat_over.append(to(mine, mine, lat_c, (0, i), me, mate))
            if nx > 1:
                side = g_lat.at[own_lat + 1, i]
                lat_side.append(to(mine, side, lat_x, (i,), my_z * nx + 1 - my_x, tp))

    lat_side = []

    def lat_last():
        for i, copy in enumerate(lat_side):
            copy.wait_recv()
            side = g_lat.at[own_lat + 1, i]
            lat_over.append(to(side, side, lat_c, (1, i), me, mate))
        for copy in lat_over:
            copy.wait_recv()

    weights = []
    for i, (source, target) in enumerate(((wg_hbm, wg), (wu_hbm, wu), (wd_hbm, wd))):
        copy = pltpu.make_async_copy(source, target, wsem.at[i])
        copy.start()
        weights.append(copy)

    class Relay:
        def __init__(self, copies, buffer, ysem, csem):
            self.copies, self.buffer, self.ysem, self.csem = copies, buffer, ysem, csem
            self.y, self.c = {}, {}

        def view(self, t, g):
            return self.buffer.at[t, pl.ds(g * per, per)]

        def spread(self, g):
            for d in range(g * per, (g + 1) * per):
                if d == 0:
                    self.copies[0].wait()
                else:
                    self.copies[d].wait_recv()
            self.y[g] = []
            for o in range(1, n_y):
                other = lax.rem(my_y + o, n_y) * CORES + my_c
                self.y[g].append(
                    to(self.view(tp, g), self.view(tp, g), self.ysem, (o, g), me, other)
                )
            self.c[g] = [to(self.view(tp, g), self.view(tp, g), self.csem, (0, g), me, mate)]

        def forward(self, g):
            for o in range(1, n_y):
                self.y[g][o - 1].wait_recv()
                came = lax.rem(my_y + n_y - o, n_y) * CORES + my_c
                self.c[g].append(
                    to(self.view(came, g), self.view(came, g), self.csem, (o, g), me, mate)
                )

        def finish(self, g):
            for copy in self.c[g]:
                copy.wait_recv()

    moe = Relay(moe_in, g_moe, moe_y, moe_c)
    block = nz * lat_ref.shape[0]
    latent = wkv_ref.shape[0]

    def expand(t, carry):
        rows = merge_rows(g_lat[t])
        kv[pl.ds(pl.multiple_of(t * block, block), block), :] = jnp.dot(
            rows[:, :latent], wkv_ref[...], preferred_element_type=jnp.float32
        ).astype(jnp.bfloat16)
        return carry

    whole_lat = g_lat.reshape(g_lat.shape[0] * block, g_lat.shape[3])
    lane = lax.broadcasted_iota(jnp.int32, (1, LANES), 1)
    packed = 2 if heads % 2 == 0 else 1
    att_in, att_mate = [], []

    def attend(part_index):
        for h in range(part_index * packed, (part_index + 1) * packed):
            head = kv[:, h * LANES : (h + 1) * LANES]
            keys = jnp.where(lane < PLAIN_HEAD_DIM, head, whole_lat[:, latent : latent + LANES])
            scores = (
                lax.dot_general(
                    q_ref[:, h * LANES : (h + 1) * LANES],
                    keys,
                    (((1,), (1,)), ((), ())),
                    preferred_element_type=jnp.float32,
                )
                * scale
            )
            top = jnp.max(scores, axis=-1, keepdims=True)
            e = jnp.exp(scores - top)
            total = jnp.sum(e, axis=-1, keepdims=True)
            mixed = (
                jnp.dot(e.astype(jnp.bfloat16), head, preferred_element_type=jnp.float32) / total
            )
            if packed == 1:
                mixed = jnp.where(lane < PLAIN_HEAD_DIM, 0.0, mixed)
            elif h % 2 == 0:
                held = pltpu.roll(mixed, VALUE_HEAD_DIM, 1)
            else:
                mixed = jnp.where(lane < VALUE_HEAD_DIM, held, mixed)
        g_att[tp, part_index] = mixed.astype(jnp.bfloat16)

    def att_send(p):
        own = g_att.at[tp, p]
        for o in range(1, n_y):
            other = lax.rem(my_y + o, n_y) * CORES + my_c
            att_in.append((p, o, to(own, own, att_y, (o, p), me, other)))
        att_mate.append(to(own, own, att_c, (0, p), me, mate))

    slots = n_ep // CHUNKS
    cap = moe_ref.shape[1]
    rows = slots * cap
    columns = moe_ref.shape[2]
    ff = wg.shape[1]
    tile = min(256, ff)

    def up(c):
        for g in range(groups):
            if (g * per) // slots == c:
                moe.finish(g)

        def one(f, carry):
            span = pl.ds(pl.multiple_of(f * tile, tile), tile)
            gate = jnp.zeros((rows, tile), jnp.float32)
            lift = jnp.zeros((rows, tile), jnp.float32)
            for t in range(n_tp):
                x = merge_rows(g_moe[t, c * slots : (c + 1) * slots])
                gate += jnp.dot(
                    x, wg[t * columns : (t + 1) * columns, span], preferred_element_type=jnp.float32
                )
                lift += jnp.dot(
                    x, wu[t * columns : (t + 1) * columns, span], preferred_element_type=jnp.float32
                )
            hidden[:, span] = (gate / (1.0 + jnp.exp(-gate)) * lift).astype(jnp.bfloat16)
            return carry

        lax.fori_loop(0, ff // tile, one, 0)

    def down(c):
        def one(t, carry):
            span = pl.ds(pl.multiple_of(t * columns, columns), columns)
            part[t, c * slots : (c + 1) * slots] = (
                jnp.dot(hidden[...], wd[:, span], preferred_element_type=jnp.float32)
                .astype(jnp.bfloat16)
                .reshape(slots, cap, columns)
            )
            return carry

        lax.fori_loop(0, n_tp, one, 0)

    reduce_c, reduce_y = {}, {}

    def swap(c):
        span = pl.ds(c * slots, slots)
        for o in list(range(1, n_y)) + [0]:
            y = lax.rem(my_y + o, n_y)
            reduce_c[c, o] = to(
                part.at[y * CORES + (1 - my_c), span], r1.at[o, span], red_c, (o, c), me, mate
            )

    def level_two(c):
        span = pl.ds(c * slots, slots)
        for o in range(1, n_y):
            y = lax.rem(my_y + o, n_y)
            reduce_c[c, o].wait_recv()
            s2[o, span] = (
                part[y * CORES + my_c, span].astype(jnp.float32) + r1[o, span].astype(jnp.float32)
            ).astype(jnp.bfloat16)
            reduce_y[c, o] = to(
                s2.at[o, span], r2.at[o, span], red_y, (o, c), me, y * CORES + my_c
            )

    returns = []

    def give_back(c):
        span = pl.ds(c * slots, slots)
        reduce_c[c, 0].wait_recv()
        total = part[tp, span].astype(jnp.float32) + r1[0, span].astype(jnp.float32)
        for o in range(1, n_y):
            reduce_y[c, o].wait_recv()
            total += r2[o, span].astype(jnp.float32)
        tot[span] = total.astype(jnp.bfloat16)
        for d in range(c * slots, (c + 1) * slots):
            if d == 0:
                back[0] = tot[0]
            else:
                returns.append(to(tot.at[d], back.at[d], ret_a, (d,), behind(d), tp))

    def att_forward():
        for p, o, copy in att_in:
            copy.wait_recv()
            came = g_att.at[lax.rem(my_y + n_y - o, n_y) * CORES + my_c, p]
            att_mate.append(to(came, came, att_c, (o, p), me, mate))

    def project():
        for copy in att_mate:
            copy.wait_recv()
        total = jnp.zeros(att_out.shape, jnp.float32)
        for t in range(n_tp):
            x = jnp.concatenate([g_att[t, p] for p in range(g_att.shape[1])], axis=1)
            width = x.shape[1]
            total += jnp.dot(
                x, wo_ref[t * width : (t + 1) * width, :], preferred_element_type=jnp.float32
            )
        att_out[...] = total.astype(jnp.bfloat16)

    parts = heads // packed
    half = groups // 2
    for g in range(half):
        moe.spread(g)
        if g > 0:
            moe.forward(g - 1)
    moe.forward(half - 1)
    moe.spread(half)
    for copy in weights:
        copy.wait()
    up(0)
    moe.forward(half)
    for g in range(half + 1, groups):
        moe.spread(g)
        moe.forward(g)
    down(0)
    swap(0)
    lat_relay(range(0, nz // 2))
    up(1)
    level_two(0)
    down(1)
    swap(1)
    lat_relay(range(nz // 2, nz))
    give_back(0)
    level_two(1)
    lat_last()
    lax.fori_loop(0, g_lat.shape[0], expand, 0)
    for p in range(parts):
        attend(p)
        if p == 0:
            give_back(1)
        att_send(p)
    att_forward()
    project()
    for copy in returns:
        copy.wait_recv()
    for copy in sends:
        copy.wait_send()


def local(
    queries,
    compressed_key_value,
    rope_key,
    latent_norm_gain,
    latent_to_key_value,
    out_proj,
    moe_input,
    moe_gain,
    routes,
    route_weight,
    gate_weight,
    up_weight,
    down_weight,
):
    n_ep = lax.axis_size("ep")
    n_tp = lax.axis_size("tp")
    me = lax.axis_index("ep")
    tp = lax.axis_index("tp")
    n_y = n_tp // CORES
    bf16 = jnp.bfloat16
    row_count = queries.shape[0]
    heads = latent_to_key_value.shape[1] // (PLAIN_HEAD_DIM + VALUE_HEAD_DIM)
    latent = compressed_key_value.shape[1]
    positions = (me * row_count + jnp.arange(row_count, dtype=jnp.int32)).astype(jnp.float32)
    q_heads = queries.reshape(row_count, heads, PLAIN_HEAD_DIM + ROPE)
    q_rope = rotary(q_heads[..., PLAIN_HEAD_DIM:].astype(jnp.float32), positions[:, None])
    pad = LANES - PLAIN_HEAD_DIM - ROPE
    q_all = jnp.concatenate(
        [
            q_heads[..., :PLAIN_HEAD_DIM],
            q_rope.astype(bf16),
            jnp.zeros((row_count, heads, pad), bf16),
        ],
        axis=-1,
    ).reshape(row_count, heads * LANES)
    share = row_count // CORES
    nx, nz, order = ep_shape(n_ep)
    cut = lambda x: lax.dynamic_slice_in_dim(x, lax.rem(tp, CORES) * share, share, 0)
    lat = jnp.concatenate(
        [
            rms_scale(cut(compressed_key_value), latent_norm_gain).astype(bf16),
            jnp.zeros((share, PLAIN_HEAD_DIM), bf16),
            rotary(cut(rope_key).astype(jnp.float32), cut(positions)).astype(bf16),
            jnp.zeros((share, pad), bf16),
        ],
        axis=1,
    )
    if heads % 2 == 0:
        wo = out_proj
        parts = heads // 2
    else:
        wo = out_proj.reshape(n_tp * heads, VALUE_HEAD_DIM, out_proj.shape[1])
        wo = jnp.concatenate([jnp.zeros_like(wo), wo], axis=1)
        wo = wo.reshape(n_tp * heads * LANES, out_proj.shape[1])
        parts = heads

    moe_rows, model_width = moe_input.shape
    top = routes.shape[1]
    capacity = 3 * moe_rows // n_ep
    places = -(-capacity // 16) * 16
    columns = model_width // n_tp
    flat = routes.reshape(-1)
    hot = (flat[:, None] == jnp.arange(n_ep, dtype=jnp.int32)[None, :]).astype(bf16)
    pairs = flat.shape[0]
    before = jnp.tril(jnp.ones((pairs, pairs), bf16), -1)
    earlier = jnp.dot(before, hot, preferred_element_type=jnp.float32)
    slot = jnp.sum(earlier * hot.astype(jnp.float32), axis=1).astype(jnp.int32)
    destination = (flat * places + slot).reshape(moe_rows, top)
    normed = rms_scale(moe_input, moe_gain).astype(bf16)
    own_normed = lax.dynamic_slice_in_dim(normed, tp * columns, columns, 1)
    place = jnp.arange(n_ep * places, dtype=jnp.int32)
    choose = jnp.zeros((n_ep * places, moe_rows), jnp.bool_)
    for k in range(top):
        choose = choose | (place[:, None] == destination[:, k][None, :])
    outgoing = jnp.dot(
        choose.astype(bf16), own_normed, preferred_element_type=jnp.float32
    ).astype(bf16)
    outgoing = outgoing.reshape(n_ep, places, columns)

    ff = gate_weight.shape[2]
    groups = min(RELAY_GROUPS, n_ep)
    vmem = pl.BlockSpec(memory_space=pltpu.VMEM)
    hbm = pl.BlockSpec(memory_space=pltpu.HBM)
    dma = lambda *shape: pltpu.SemaphoreType.DMA((2,) + shape)
    attention_out, back = pl.pallas_call(
        functools.partial(fused, n_ep, n_tp, heads, (PLAIN_HEAD_DIM + ROPE) ** (-0.5)),
        out_shape=(
            jax.ShapeDtypeStruct((row_count, out_proj.shape[1]), bf16),
            jax.ShapeDtypeStruct((n_ep, places, columns), bf16),
        ),
        in_specs=[vmem] * 5 + [hbm] * 3,
        out_specs=(vmem, vmem),
        scratch_shapes=[
            pltpu.VMEM((model_width, ff), bf16),
            pltpu.VMEM((model_width, ff), bf16),
            pltpu.VMEM((ff, model_width), bf16),
            pltpu.VMEM((CORES * nx, nz, share, latent + LANES), bf16),
            pltpu.VMEM((n_tp, n_ep, places, columns), bf16),
            pltpu.VMEM((n_tp, parts, row_count, LANES), bf16),
            pltpu.VMEM((n_ep * row_count, heads * LANES), bf16),
            pltpu.VMEM((n_ep // CHUNKS * places, ff), bf16),
            pltpu.VMEM((n_tp, n_ep, places, columns), bf16),
            pltpu.VMEM((n_y, n_ep, places, columns), bf16),
            pltpu.VMEM((n_y, n_ep, places, columns), bf16),
            pltpu.VMEM((n_y, n_ep, places, columns), bf16),
            pltpu.VMEM((n_ep, places, columns), bf16),
            pltpu.SemaphoreType.DMA((3,)),
            pltpu.SemaphoreType.DMA((2,)),
            dma(nz),
            dma(nz),
            dma(nx, nz),
            dma(n_ep),
            dma(n_y, groups),
            dma(n_y, groups),
            dma(n_y, parts),
            dma(n_y, parts),
            dma(n_y, CHUNKS),
            dma(n_y, CHUNKS),
            dma(n_ep),
        ],
        compiler_params=pltpu.CompilerParams(
            collective_id=0, has_side_effects=True, vmem_limit_bytes=60 * 1024 * 1024
        ),
        name="fused",
    )(
        q_all,
        lat,
        latent_to_key_value,
        wo,
        outgoing,
        gate_weight.reshape(model_width, ff),
        up_weight.reshape(model_width, ff),
        down_weight.reshape(ff, model_width),
    )
    flat_back = back.reshape(n_ep * places, columns)
    far = lax.rem(routes // nx - me // nx + nz, nz)
    step = jnp.zeros_like(far)
    for i, dz in enumerate(order):
        step = jnp.where(far == dz, i, step)
    side = lax.rem(routes % nx - me % nx + nx, nx)
    near = (step * nx + side) * places + slot.reshape(moe_rows, top)
    expert_out = jnp.zeros((moe_rows, columns), jnp.float32)
    for k in range(top):
        pick = (near[:, k][:, None] == place[None, :]).astype(bf16)
        picked = jnp.dot(pick, flat_back, preferred_element_type=jnp.float32)
        expert_out = expert_out + picked * route_weight[:, k][:, None]
    return (attention_out, expert_out.astype(bf16))


def solution(mesh):
    return jax.shard_map(
        local,
        mesh=mesh,
        in_specs=(
            P("ep", "tp"),
            P("ep", None),
            P("ep", None),
            P(),
            P(None, "tp"),
            P(None, "tp"),
            P("ep", None),
            P(),
            P("ep", None),
            P("ep", None),
            P("ep", None, "tp"),
            P("ep", None, "tp"),
            P("ep", "tp", None),
        ),
        out_specs=(P("ep", "tp"), P("ep", "tp")),
        check_vma=False,
    )
```
